512 devices in a mesh: kv: 128 (over z, y, core), tp: 4 (over x).
Axes of the slice: x: 4, y: 8, z: 8, core: 2. Of those that a mesh axis runs over, the one named last changes fastest.
Arguments:
- piece_tokens: bfloat16 [512, 2048], P('kv'), may hold values from -6 to 6
- decode_tokens: bfloat16 [128, 2048], P('kv'), may hold values from -6 to 6
- prompt_fill: int32 [1], replicated, may hold values from 16384 to 32256
- decode_fill: int32 [128], P('kv'), may hold values from 1 to 767, 49152 in all
- prompt_cache: bfloat16 [32768, 544], P('kv'), may hold values from -600 to 600
- decode_cache: bfloat16 [128, 768, 544], P('kv'), may hold values from -600 to 600
- input_gain: float32 [2048], replicated, may hold values from 0.1 to 1.9
- query_gain: float32 [768], replicated, may hold values from 0.1 to 1.9
- latent_gain: float32 [512], replicated, may hold values from 0.1 to 1.9
- query_down: bfloat16 [2048, 768], P(None, 'tp'), may hold values from -0.125 to 0.125
- latent_down: bfloat16 [2048, 512], P(None, 'tp'), may hold values from -0.125 to 0.125
- rope_down: bfloat16 [2048, 32], replicated, may hold values from -0.125 to 0.125
- query_up: bfloat16 [768, 1024], P(None, 'tp'), may hold values from -0.21875 to 0.21875
- qrope_up: bfloat16 [768, 512], P(None, 'tp'), may hold values from -0.21875 to 0.21875
- key_up: bfloat16 [16, 64, 512], P('tp'), may hold values from -0.25 to 0.25
- value_up: bfloat16 [16, 512, 64], P('tp'), may hold values from -4 to 4
- out_proj: bfloat16 [1024, 2048], P('tp'), may hold values from -4 to 4
Outputs:
- piece_out: bfloat16 [512, 2048], P('kv')
- decode_out: bfloat16 [128, 2048], P('kv')
- piece_rows: bfloat16 [512, 544], P('kv')
- decode_rows: bfloat16 [128, 544], P('kv')
The draws below stay inside these ranges and needn't reach their ends.
Inputs may be any that keep to these rules, and one draw needn't show every extreme that they name: `prompt_fill`: the piece takes the 512 positions that follow the cache's filled positions. `decode_fill`: a decoding sequence's new token takes the position that follows its filled ones.
All inputs are finite; a program needn't handle non-finite values. No bound on the sum of `decode_fill` on one device may be relied on, other than what follows from the above.
Results may differ from the reference program's by a relative error of at most 0.035.
Values may be sent and summed in bfloat16 or wider, within the bound.
No kernel may reach another device: no remote copies, remote signals or barrier semaphores. Data moves between devices by JAX's collectives and lax.ppermute only.
A program may use at most 64 MiB of HBM per device.

```python
import math
import jax
import jax.numpy as jnp
import numpy as np
from jax import lax

D = 2048
H = 16
QL = 768
KL = 512
NOPE = 64
ROPE = 32
VD = 64
CACHE_DEV = 256
DEC_LEN = 768
PIECE = 512
CACHE = 32768
DEC = 128
N_KV = 128
N_TP = 4


def draw_prompt_cache(key, part):
    values = jnp.clip(jax.random.normal(key, (CACHE, KL + ROPE), jnp.float32), -5.0, 5.0)
    return values.astype(jnp.bfloat16)


def draw_decode_cache(key, part):
    values = jnp.clip(jax.random.normal(key, (DEC, DEC_LEN, KL + ROPE), jnp.float32), -5.0, 5.0)
    return values.astype(jnp.bfloat16)


def block_levels(key, dims, pieces, least, largest):
    def one(position, shards_of):
        draws = jax.random.uniform(jax.random.fold_in(jax.random.fold_in(key, 6), position), (shards_of,), jnp.float32, least / len(pieces), largest / len(pieces))
        return jnp.repeat(jnp.exp(draws), dims[position] // shards_of).reshape((-1,) + (1,) * (len(dims) - position - 1))

    gain = one(*pieces[0])
    for cut in pieces[1:]:
        gain = gain * one(*cut)
    return gain


def profile(amount, total, most, slope):
    weights = [(1 << 20) // math.isqrt(grade ** slope) + 1 for grade in range(2, amount + 1)]
    rest, holding = total - most - (amount - 1), [1] * (amount - 1)
    while rest > 0:
        candidates = [i for i in range(amount - 1) if holding[i] < most]
        whole, left = sum([weights[i] for i in candidates]), rest
        for i in candidates:
            extra = min(most - holding[i], max(1, left * weights[i] // whole), rest)
            holding[i] = holding[i] + extra
            rest = rest - extra
    return np.array([most] + holding)


def uneven(rng, amount, total, most, skew):
    if amount == 2:
        one = jax.random.randint(rng, (), max(1, total - most), min(most, total - 1) + 1)
        return jnp.stack([one, total - one])
    tallies = jnp.asarray(profile(amount, total, most, skew), jnp.int32)
    couples = (amount - 1) // 2
    donor, receiver = tallies[1:1 + 2 * couples:2], tallies[2:2 + 2 * couples:2]
    margin = jnp.minimum(donor - 1, most - receiver)
    moved = jax.random.randint(jax.random.fold_in(rng, 1), (couples,), 0, 1 << 20) % (margin + 1)
    tallies = tallies.at[1:1 + 2 * couples:2].set(donor - moved).at[2:2 + 2 * couples:2].set(receiver + moved)
    return tallies[jax.random.permutation(jax.random.fold_in(rng, 2), amount)]


def gaussian(stream_key, dims, scale, most, split=(), held_as=jnp.bfloat16):
    result = scale * jax.random.normal(stream_key, dims, jnp.float32)
    if split:
        result = result * block_levels(stream_key, dims, split, -0.22, 0.18)
    return jnp.clip(result, -most, most).astype(held_as)


def setup_inputs(seed: int = 0) -> dict:
    key_of = jax.random.split(jax.random.key(seed), 18)
    return {
        "piece_tokens": gaussian(key_of[0], (PIECE, D), 1.0, 6.0, ((0, 128),)),
        "decode_tokens": gaussian(key_of[1], (DEC, D), 1.0, 6.0, ((0, 128),)),
        "prompt_fill": jax.random.randint(key_of[2], (1,), CACHE // 2, CACHE - PIECE + 1).astype(jnp.int32),
        "decode_fill": uneven(key_of[3], DEC, DEC * DEC_LEN // 2, DEC_LEN - 1, 2).astype(jnp.int32),
        "prompt_cache": draw_prompt_cache(jax.random.fold_in(key_of[17], 71), 0),
        "decode_cache": draw_decode_cache(jax.random.fold_in(key_of[17], 71), 0),
        "input_gain": jnp.clip(1.0 + 0.18 * jax.random.normal(key_of[6], (D,), jnp.float32), 0.1, 1.9),
        "query_gain": jnp.clip(1.0 + 0.18 * jax.random.normal(key_of[7], (QL,), jnp.float32), 0.1, 1.9),
        "latent_gain": jnp.clip(1.0 + 0.18 * jax.random.normal(key_of[8], (KL,), jnp.float32), 0.1, 1.9),
        "query_down": gaussian(key_of[9], (D, QL), D ** -0.5, 0.125, ((1, 4),)),
        "latent_down": gaussian(key_of[10], (D, KL), D ** -0.5, 0.125, ((1, 4),)),
        "rope_down": gaussian(key_of[11], (D, ROPE), D ** -0.5, 0.125),
        "query_up": gaussian(key_of[12], (QL, H * NOPE), QL ** -0.5, 0.21875, ((1, 4),)),
        "qrope_up": gaussian(key_of[13], (QL, H * ROPE), QL ** -0.5, 0.21875, ((1, 4),)),
        "key_up": gaussian(key_of[14], (H, NOPE, KL), KL ** -0.5, 0.25, ((0, 4),)),
        "value_up": gaussian(key_of[15], (H, KL, VD), 0.25, 4.0, ((0, 4),)),
        "out_proj": gaussian(key_of[16], (H * VD, D), 0.25, 4.0, ((0, 4),)),
    }


NEG_FILL = -1e+30
RMS_EPS = 1e-06
THETA = 10000.0

def rms_scale(values, gain_row):
    widened = values.astype(jnp.float32)
    scaled = widened * lax.rsqrt(lax.optimization_barrier(jnp.mean(widened * widened, axis=-1, keepdims=True)) + RMS_EPS) * gain_row.astype(jnp.float32)
    return scaled.astype(jnp.bfloat16)

def rotate(values, places):
    half_width = values.shape[-1] // 2
    inverse = THETA ** (-jnp.arange(half_width, dtype=jnp.float32) / half_width)
    angles = places.astype(jnp.float32)[..., None] * inverse
    first_half = values[..., :half_width].astype(jnp.float32)
    second_half = values[..., half_width:].astype(jnp.float32)
    cosine = jnp.cos(angles)
    sine_part = jnp.sin(angles)
    return jnp.concatenate([first_half * cosine - second_half * sine_part, first_half * sine_part + second_half * cosine], axis=-1).astype(jnp.bfloat16)

def project(tokens, places, input_gain, query_gain, latent_gain, query_down, latent_down, rope_down):
    normed = rms_scale(tokens, input_gain)
    query_comp = jnp.dot(normed, query_down, preferred_element_type=jnp.float32).astype(jnp.bfloat16)
    latent_comp = jnp.dot(normed, latent_down, preferred_element_type=jnp.float32).astype(jnp.bfloat16)
    rope_raw = jnp.dot(normed, rope_down, preferred_element_type=jnp.float32).astype(jnp.bfloat16)
    new_rows = jnp.concatenate([rms_scale(latent_comp, latent_gain), rotate(rope_raw, places)], axis=-1)
    return (rms_scale(query_comp, query_gain), new_rows)

def make_queries(query_lat, places, query_up, qrope_up, key_up):
    row_count = query_lat.shape[0]
    head_count = key_up.shape[0]
    nope_part = jnp.dot(query_lat, query_up, preferred_element_type=jnp.float32).astype(jnp.bfloat16).reshape(row_count, head_count, -1)
    rope_raw = jnp.dot(query_lat, qrope_up, preferred_element_type=jnp.float32).astype(jnp.bfloat16).reshape(row_count, head_count, -1)
    turned = rotate(rope_raw, places[:, None])
    absorbed = jnp.einsum('nhc,hcl->nhl', nope_part.astype(jnp.float32), key_up.astype(jnp.float32)).astype(jnp.bfloat16)
    return (absorbed, turned)

def block_attend(absorbed, turned, key_rows, key_places, query_places, value_up):
    latent_width = value_up.shape[1]
    score_scale = (NOPE + ROPE) ** (-0.5)
    latent_keys = key_rows[:, :latent_width].astype(jnp.float32)
    scores = (jnp.einsum('nhl,sl->nhs', absorbed.astype(jnp.float32), latent_keys) + jnp.einsum('nhr,sr->nhs', turned.astype(jnp.float32), key_rows[:, latent_width:].astype(jnp.float32))) * score_scale
    allowed = key_places[None, None, :] <= query_places[:, None, None]
    scores = jnp.where(allowed, scores, NEG_FILL)
    local_peak = lax.optimization_barrier(jnp.max(scores, axis=-1))
    exp_scores = jnp.where(allowed, jnp.exp(scores - local_peak[..., None]), 0.0)
    weight_sum = lax.optimization_barrier(jnp.sum(exp_scores, axis=-1))
    weights = lax.optimization_barrier(exp_scores.astype(jnp.bfloat16)).astype(jnp.float32)
    mixed_rows = jnp.einsum('nhs,sl->nhl', weights, latent_keys)
    partial_sum = jnp.einsum('nhl,hlv->nhv', mixed_rows, value_up.astype(jnp.float32), precision=lax.Precision.HIGHEST)
    return (partial_sum, weight_sum, local_peak)

def insert_row(cache_rows, new_row, fill_one):
    return lax.dynamic_update_slice(cache_rows, new_row[None], (fill_one.astype(jnp.int32), jnp.zeros((), jnp.int32)))

def project_out(values, out_proj):
    row_count = values.shape[0]
    grouped = values.reshape(row_count, N_TP, -1).astype(jnp.float32)
    weight_groups = out_proj.reshape(N_TP, -1, out_proj.shape[1]).astype(jnp.float32)
    group_out = jnp.einsum('ngk,gkd->ngd', grouped, weight_groups).astype(jnp.bfloat16)
    group_out = lax.optimization_barrier(group_out).astype(jnp.float32)
    return lax.optimization_barrier(jnp.sum(group_out, axis=1)).astype(jnp.bfloat16)

def reference(piece_tokens, decode_tokens, prompt_fill, decode_fill, prompt_cache, decode_cache, input_gain, query_gain, latent_gain, query_down, latent_down, rope_down, query_up, qrope_up, key_up, value_up, out_proj):
    fill_start = prompt_fill[0].astype(jnp.int32)
    piece_places = fill_start + jnp.arange(PIECE, dtype=jnp.int32)
    decode_places = decode_fill.astype(jnp.int32)
    piece_lat, piece_rows = project(piece_tokens, piece_places, input_gain, query_gain, latent_gain, query_down, latent_down, rope_down)
    decode_lat, decode_rows = project(decode_tokens, decode_places, input_gain, query_gain, latent_gain, query_down, latent_down, rope_down)
    piece_absorbed, piece_turned = make_queries(piece_lat, piece_places, query_up, qrope_up, key_up)
    decode_absorbed, decode_turned = make_queries(decode_lat, decode_places, query_up, qrope_up, key_up)
    full_cache = lax.dynamic_update_slice(prompt_cache, piece_rows, (fill_start, jnp.zeros((), jnp.int32)))
    head_count = key_up.shape[0]
    value_width = value_up.shape[2]

    def step(carry, block_index):
        peak_run, numer_run, denom_run = carry
        key_rows = lax.dynamic_slice_in_dim(full_cache, block_index * CACHE_DEV, CACHE_DEV, 0)
        key_places = block_index * CACHE_DEV + jnp.arange(CACHE_DEV, dtype=jnp.int32)
        partial_sum, weight_sum, local_peak = block_attend(piece_absorbed, piece_turned, key_rows, key_places, piece_places, value_up)
        new_peak = jnp.maximum(peak_run, local_peak)
        old_factor = jnp.exp(peak_run - new_peak)
        new_factor = jnp.exp(local_peak - new_peak)
        numer_run = numer_run * old_factor[..., None] + partial_sum * new_factor[..., None]
        denom_run = denom_run * old_factor + weight_sum * new_factor
        return ((new_peak, numer_run, denom_run), None)
    start_carry = (jnp.full((PIECE, head_count), NEG_FILL, jnp.float32), jnp.zeros((PIECE, head_count, value_width), jnp.float32), jnp.zeros((PIECE, head_count), jnp.float32))
    final_carry, unused = lax.scan(step, start_carry, jnp.arange(N_KV, dtype=jnp.int32))
    piece_value = (final_carry[1] / final_carry[2][..., None]).astype(jnp.bfloat16)
    decode_keys = jax.vmap(insert_row)(decode_cache, decode_rows, decode_places)

    def attend_one(absorbed_one, turned_one, keys_one, fill_one):
        key_places = jnp.arange(keys_one.shape[0], dtype=jnp.int32)
        return block_attend(absorbed_one[None], turned_one[None], keys_one, key_places, fill_one[None], value_up)
    decode_part, decode_total, decode_peak = jax.vmap(attend_one)(decode_absorbed, decode_turned, decode_keys, decode_places)
    decode_value = (decode_part[:, 0] / decode_total[:, 0, :, None]).astype(jnp.bfloat16)
    piece_out = project_out(piece_value.reshape(PIECE, -1), out_proj)
    decode_out = project_out(decode_value.reshape(decode_value.shape[0], -1), out_proj)
    return (piece_out, decode_out, piece_rows, decode_rows)
```

```python
import jax
import jax.numpy as jnp
import numpy as np
from jax import lax
from jax.experimental import pallas as pl
from jax.experimental.pallas import tpu as pltpu
from jax.sharding import Mesh, PartitionSpec as P

NOPE = 64
ROPE = 32
NEG_FILL = -1e30
RMS_EPS = 1e-06
THETA = 10000.0
SCALE = (NOPE + ROPE) ** (-0.5)
TP = 4
PIECE_DEV = 4
BF = jnp.bfloat16
F32 = jnp.float32

GROUP = ("core",)
REST = ("z", "yh", "yl")
KV = ("z", "yh", "yl", "core")


def dot(a, b):
    return lax.dot_general(a, b, (((1,), (0,)), ((), ())), preferred_element_type=F32)


def dot_t(a, b):
    return lax.dot_general(a, b, (((1,), (1,)), ((), ())), preferred_element_type=F32)


def swap_matrix():
    rows = lax.broadcasted_iota(jnp.int32, (128, 128), 0)
    columns = lax.broadcasted_iota(jnp.int32, (128, 128), 1)
    return (rows == columns + jnp.where(columns % 32 < 16, 16, -16)).astype(BF)


def angle_tables(places):
    half = ROPE // 2
    inverse = THETA ** (-jnp.arange(half, dtype=F32) / half)
    angles = places.astype(F32)[:, None] * inverse
    cosine, sine = jnp.cos(angles), jnp.sin(angles)
    cos_table = jnp.concatenate([cosine, cosine] * TP, axis=-1)
    sin_table = jnp.concatenate([-sine, sine] * TP, axis=-1)
    return cos_table, sin_table


def turn(raw, cos_table, sin_table):
    swapped = dot(raw, swap_matrix())
    return (raw.astype(F32) * cos_table + swapped * sin_table).astype(BF)


def rms(values, gain):
    mean = jnp.mean(values * values, axis=-1, keepdims=True)
    return (values * lax.rsqrt(mean + RMS_EPS) * gain).astype(BF)


def head_lanes(width, rows):
    return lax.broadcasted_iota(jnp.int32, (rows, TP * width), 1) // width


def project_kernel(tokens, gain, query_t, latent, rope_t, cos_table, sin_table, out):
    normed = rms(tokens[...].astype(F32), gain[...])
    query = dot_t(normed, query_t[...])
    lat = dot(normed, latent[...])
    raw = dot_t(normed, rope_t[...]).astype(BF)
    raw = jnp.concatenate([raw.astype(F32)] * 4, axis=-1).astype(BF)
    turned = turn(raw, cos_table[...], sin_table[...])
    out[:, 0:192] = query.astype(BF)
    out[:, 256:384] = lat.astype(BF)
    out[:, 384:512] = turned


def rows_kernel(group, own, arrived, query_gain, latent_gain, query_out, rows_out, ropes_out):
    mine = own[0]
    parts = [arrived[mine * TP + p, :, 0:192].astype(F32) for p in range(TP)]
    query_out[...] = rms(jnp.concatenate(parts, axis=-1), query_gain[...])
    for j in range(group):
        parts = [arrived[j * TP + p, :, 256:384].astype(F32) for p in range(TP)]
        rows_out[j] = rms(jnp.concatenate(parts, axis=-1), latent_gain[...])
        ropes_out[j] = arrived[j * TP, :, 384:512]


def make_queries(query_lat, cos_table, sin_table, query_up, qrope_up):
    nope = dot(query_lat, query_up).astype(BF)
    raw = dot(query_lat, qrope_up).astype(BF)
    return nope, turn(raw, cos_table, sin_table)


def masked_to(values, width, head):
    lanes = head_lanes(width, values.shape[0])
    return jnp.where(lanes == head, values.astype(F32), 0.0).astype(BF)


def piece_kernel(group, rows, *refs):
    scalars, query_lat, cos_table, sin_table, query_up, qrope_up, key_up, value_up = refs[:8]
    caches = refs[8 : 8 + group]
    fresh, fresh_rope, out = refs[8 + group :]
    fill, own, rest = scalars[0], scalars[1], scalars[2]
    span = caches[0].shape[1]
    nope, turned = make_queries(
        query_lat[...], cos_table[...], sin_table[...], query_up[...], qrope_up[...]
    )
    fresh_keys = fresh[...]
    fresh_count = fresh_keys.shape[0]
    token = lax.broadcasted_iota(jnp.int32, (rows, fresh_count), 0)
    slot = lax.broadcasted_iota(jnp.int32, (rows, fresh_count), 1)
    query_rel = ((token // PIECE_DEV) * group + own) * PIECE_DEV + token % PIECE_DEV
    key_rel = (rest * group + slot // 8) * PIECE_DEV + slot % 8
    fresh_allowed = (slot % 8 < PIECE_DEV) & (key_rel <= query_rel)
    column = lax.broadcasted_iota(jnp.int32, (1, span), 1)
    keys = [c[0:512, :] for c in caches]
    ropes = [
        jnp.concatenate([c[512:544, :]] * TP, axis=0) for c in caches
    ]
    allowed = [column + scalars[3 + j] < fill for j in range(group)]
    values = jnp.zeros((rows, 256), F32)
    stats = jnp.zeros((rows, 128), F32)
    lane = lax.broadcasted_iota(jnp.int32, (rows, 128), 1)
    value_lanes = head_lanes(64, rows)
    for head in range(TP):
        absorbed = dot(masked_to(nope, 64, head), key_up[...]).astype(BF)
        turned_one = masked_to(turned, 32, head)
        scores = [
            jnp.where(ok, (dot(absorbed, k) + dot(turned_one, r)) * SCALE, NEG_FILL)
            for k, r, ok in zip(keys, ropes, allowed)
        ]
        extra = (dot_t(absorbed, fresh_keys) + dot_t(turned_one, fresh_rope[...])) * SCALE
        extra = jnp.where(fresh_allowed, extra, NEG_FILL)
        peak = jnp.max(extra, axis=-1, keepdims=True)
        for s in scores:
            peak = jnp.maximum(peak, jnp.max(s, axis=-1, keepdims=True))
        total = jnp.zeros((rows, 1), F32)
        mixed = jnp.zeros((rows, 512), F32)
        for s, k, ok in zip(scores, keys, allowed):
            weights = jnp.where(ok, jnp.exp(s - peak), 0.0)
            total = total + jnp.sum(weights, axis=-1, keepdims=True)
            mixed = mixed + dot_t(weights.astype(BF), k)
        weights = jnp.where(fresh_allowed, jnp.exp(extra - peak), 0.0)
        total = total + jnp.sum(weights, axis=-1, keepdims=True)
        mixed = mixed + dot(weights.astype(BF), fresh_keys)
        some = total > 0.0
        safe = jnp.where(some, total, 1.0)
        mixed = (mixed * (1.0 / safe)).astype(BF)
        level = jnp.where(some, peak + jnp.log(safe), NEG_FILL)
        values = jnp.where(value_lanes == head, dot_t(mixed, value_up[...]), values)
        rest_of = level
        for piece in range(3):
            part = rest_of.astype(BF).astype(F32)
            stats = jnp.where(lane == 3 * head + piece, part, stats)
            rest_of = rest_of - part
    out[:, 0:256] = values.astype(BF)
    out[:, 256:384] = stats.astype(BF)


def decode_kernel(scalars, query_lat, cos_table, sin_table, query_up, qrope_up, key_up,
                  value_up, cache, row, row_rope, out):
    fill = scalars[0]
    nope, turned = make_queries(
        query_lat[...], cos_table[...], sin_table[...], query_up[...], qrope_up[...]
    )
    nope, turned = nope.astype(F32)[0:1], turned.astype(F32)[0:1]
    head = lax.broadcasted_iota(jnp.int32, (8, 256), 0)
    nope = jnp.where(head_lanes(64, 8) == head, nope, 0.0).astype(BF)
    head = lax.broadcasted_iota(jnp.int32, (8, 128), 0)
    turned = jnp.where(head_lanes(32, 8) == head, turned, 0.0).astype(BF)
    absorbed = dot(nope, key_up[...]).astype(BF)
    keys = cache[0:512, :]
    ropes = jnp.concatenate([cache[512:544, :]] * TP, axis=0)
    span = cache.shape[1]
    allowed = lax.broadcasted_iota(jnp.int32, (8, span), 1) < fill
    scores = jnp.where(allowed, (dot(absorbed, keys) + dot(turned, ropes)) * SCALE, NEG_FILL)
    own = row[...].astype(F32)
    extra = jnp.sum(absorbed.astype(F32) * own, axis=-1, keepdims=True)
    extra += jnp.sum(turned.astype(F32) * row_rope[...].astype(F32), axis=-1, keepdims=True)
    extra = extra * SCALE
    peak = jnp.maximum(jnp.max(scores, axis=-1, keepdims=True), extra)
    weights = jnp.where(allowed, jnp.exp(scores - peak), 0.0)
    weight = jnp.exp(extra - peak)
    total = jnp.sum(weights, axis=-1, keepdims=True) + weight
    mixed = dot_t(weights.astype(BF), keys) + weight * own
    mixed = (mixed / total).astype(BF)
    projected = dot_t(mixed, value_up[...])
    head = lax.broadcasted_iota(jnp.int32, (8, 256), 0)
    projected = jnp.where(head_lanes(64, 8) == head, projected, 0.0)
    out[...] = jnp.sum(projected, axis=0, keepdims=True)


def merge_kernel(arrived, decode_value, out_proj, out):
    count = arrived.shape[0]
    source = lax.broadcasted_iota(jnp.int32, (128, 256), 0)
    target = lax.broadcasted_iota(jnp.int32, (128, 256), 1)
    spread = ((source // 3 == target // 64) & (source < 12)).astype(BF)
    level = dot(arrived[:, 256:384], spread).reshape(count // 8, 8, 256)
    values = arrived[:, 0:256].astype(F32).reshape(count // 8, 8, 256)
    top = jnp.max(level, axis=0)
    top = jnp.maximum(top, pltpu.roll(top, 4, 0))
    factor = jnp.exp(level - top[None])
    numer = jnp.sum(factor * values, axis=0)
    denom = jnp.sum(factor, axis=0)
    numer = numer + pltpu.roll(numer, 4, 0)
    denom = denom + pltpu.roll(denom, 4, 0)
    row = lax.broadcasted_iota(jnp.int32, (8, 256), 0)
    merged = jnp.where(row < 4, numer / denom, decode_value[...]).astype(BF)
    out[...] = dot(merged, out_proj[...]).astype(BF)


def call(kernel, out_shapes, operands, smem=(), flops=10**7):
    specs = [
        pl.BlockSpec(memory_space=pltpu.SMEM if k in smem else pltpu.VMEM)
        for k in range(len(operands))
    ]
    many = isinstance(out_shapes, (list, tuple))
    vmem = pl.BlockSpec(memory_space=pltpu.VMEM)
    size = sum(o.size * o.dtype.itemsize for o in operands)
    return pl.pallas_call(
        kernel,
        out_shape=out_shapes,
        in_specs=specs,
        out_specs=[vmem] * len(out_shapes) if many else vmem,
        cost_estimate=pl.CostEstimate(flops=flops, bytes_accessed=size, transcendentals=0),
    )(*operands)


def from_everyone(shard, axes):
    count = lax.axis_size(axes)
    copies = jnp.broadcast_to(shard, (count, *shard.shape))
    return lax.all_to_all(copies, axes, split_axis=0, concat_axis=0, tiled=True)


def local(
    piece_tokens,
    decode_tokens,
    prompt_fill,
    decode_fill,
    prompt_cache,
    decode_cache,
    input_gain,
    query_gain,
    latent_gain,
    query_down,
    latent_down,
    rope_down,
    query_up,
    qrope_up,
    key_up,
    value_up,
    out_proj,
):
    kv_index = lax.axis_index(KV)
    own = lax.axis_index(GROUP)
    rest = lax.axis_index(REST)
    group = lax.axis_size(GROUP)
    rest_count = lax.axis_size(REST)
    rows = rest_count * PIECE_DEV
    fill = prompt_fill[0]
    span = prompt_cache.shape[0]

    cache_t = prompt_cache.T
    caches = [cache_t, lax.ppermute(cache_t, "core", [(0, 1), (1, 0)])]
    bases = [kv_index * span, (rest * group + 1 - own) * span]

    step = jnp.arange(8, dtype=jnp.int32)
    places = jnp.where(step < PIECE_DEV, fill + kv_index * PIECE_DEV + step, decode_fill[0])
    cos_own, sin_own = angle_tables(places)
    tokens = jnp.concatenate([piece_tokens, decode_tokens, jnp.zeros((3, 2048), BF)], axis=0)
    packed = call(
        project_kernel,
        jax.ShapeDtypeStruct((8, 512), BF),
        (tokens, input_gain[None], query_down.T, latent_down, rope_down.T, cos_own, sin_own),
    )
    arrived = from_everyone(packed, GROUP + ("tp",))
    query_lat, new_rows, new_ropes = call(
        lambda *refs: rows_kernel(group, *refs),
        [
            jax.ShapeDtypeStruct((8, 768), BF),
            jax.ShapeDtypeStruct((group, 8, 512), BF),
            jax.ShapeDtypeStruct((group, 8, 128), BF),
        ],
        (own[None], arrived, query_gain[None], latent_gain[None]),
        smem=(0,),
    )
    own_rows = jnp.concatenate(
        [
            lax.dynamic_index_in_dim(new_rows, own, 0, keepdims=False),
            lax.dynamic_index_in_dim(new_ropes, own, 0, keepdims=False)[:, :ROPE],
        ],
        axis=-1,
    )

    piece_lat = from_everyone(query_lat[:PIECE_DEV], REST).reshape(rows, -1)

    key_flat = key_up.reshape(TP * NOPE, -1)
    value_flat = jnp.swapaxes(value_up, 1, 2).reshape(TP * 64, -1)
    decode_row = lax.dynamic_index_in_dim(new_rows, own, 0, keepdims=False)[4:5]
    decode_rope = lax.dynamic_index_in_dim(new_ropes, own, 0, keepdims=False)[4:5]
    decode_lat = jnp.broadcast_to(query_lat[4:5], query_lat.shape)
    decode_value = call(
        decode_kernel,
        jax.ShapeDtypeStruct((1, 256), F32),
        (
            decode_fill,
            decode_lat,
            cos_own[4:5],
            sin_own[4:5],
            query_up,
            qrope_up,
            key_flat,
            value_flat,
            decode_cache[0].T,
            decode_row,
            decode_rope,
        ),
        smem=(0,),
    )

    token = jnp.arange(rows, dtype=jnp.int32)
    class_places = fill + ((token // PIECE_DEV) * group + own) * PIECE_DEV + token % PIECE_DEV
    cos_class, sin_class = angle_tables(class_places)
    scalars = jnp.stack([fill, own, rest, *bases]).astype(jnp.int32)
    partial = call(
        lambda *refs: piece_kernel(group, rows, *refs),
        jax.ShapeDtypeStruct((rows, 384), BF),
        (
            scalars,
            piece_lat,
            cos_class,
            sin_class,
            query_up,
            qrope_up,
            key_flat,
            value_flat,
            *caches,
            new_rows.reshape(group * 8, -1),
            new_ropes.reshape(group * 8, -1),
        ),
        smem=(0,),
        flops=3 * 10**9,
    )
    returned = lax.all_to_all(
        partial.reshape(rest_count, PIECE_DEV, -1), REST, split_axis=0, concat_axis=0, tiled=True
    ).reshape(rows, -1)
    group_out = call(
        merge_kernel,
        jax.ShapeDtypeStruct((8, 2048), BF),
        (returned, decode_value, out_proj),
    )
    everyone = from_everyone(group_out, "tp")
    summed = jnp.sum(everyone.astype(F32), axis=0).astype(BF)
    return (summed[:PIECE_DEV], summed[PIECE_DEV : PIECE_DEV + 1], own_rows[:PIECE_DEV],
            own_rows[PIECE_DEV : PIECE_DEV + 1])


def solution(mesh):
    split = Mesh(mesh.devices.reshape(8, 4, 2, 2, TP), ("z", "yh", "yl", "core", "tp"))
    placed = (
        P(KV, None),
        P(KV, None),
        P(),
        P(KV),
        P(KV, None),
        P(KV, None, None),
        P(),
        P(),
        P(),
        P(None, "tp"),
        P(None, "tp"),
        P(),
        P(None, "tp"),
        P(None, "tp"),
        P("tp", None, None),
        P("tp", None, None),
        P("tp", None),
    )
    return jax.shard_map(
        local,
        mesh=split,
        in_specs=placed,
        out_specs=(P(KV, None), P(KV, None), P(KV, None), P(KV, None)),
        check_vma=False,
    )
```
